32 devices in a mesh: grp: 2 (over y), sp: 4 (over z), tp: 4 (over x, core).
Axes of the slice: x: 2, y: 2, z: 4, core: 2. Of those that a mesh axis runs over, the one named last changes fastest.
Arguments:
- carryover_vector: bfloat16 [2048, 2048], P(('grp', 'sp', 'tp')), parts along dimension 0, may hold values from -6 to 6
- channel_source_entries: bfloat16 [2048, 1024], P(('grp', 'sp'), 'tp'), parts along dimension 0, may hold values from -6 to 6
- final_modulation_vector: bfloat16 [2048, 1024], P(('grp', 'sp'), 'tp'), parts along dimension 0, may hold values from -54 to 54
- entering_basis_matrix: bfloat16 [2048, 512], P(('grp', 'sp'), 'tp'), parts along dimension 0, may hold values from -6 to 6
- readout_basis_matrix: bfloat16 [2048, 512], P(('grp', 'sp'), 'tp'), parts along dimension 0, may hold values from -6 to 6
- raw_stride_amount: float32 [2048, 16], P(('grp', 'sp'), 'tp'), parts along dimension 0, may hold values from -6 to 5
- extra_log_attenuation: float32 [2048, 16], P(('grp', 'sp'), 'tp'), parts along dimension 0, may hold values from -1.4 to 0
- channel_fading_rate: float32 [16], P('tp'), may hold values from 0 to 0.1, as said below
- channel_source_kernel: float32 [4, 1024], P(None, 'tp'), may hold values from -3 to 3
- entering_basis_kernel: float32 [4, 512], P(None, 'tp'), may hold values from -3 to 3
- readout_basis_kernel: float32 [4, 512], P(None, 'tp'), may hold values from -3 to 3
- modulated_rescaling_vector: float32 [1024], replicated, may hold values from 0.1 to 1.9
- blender_final_matrix: bfloat16 [1024, 2048], replicated, may hold values from -0.1875 to 0.1875
- specialist_rescaling_vector: float32 [2048], replicated, may hold values from 0.1 to 1.9
- specialist_gating_matrices: bfloat16 [8, 2048, 1024], P('sp', None, 'tp'), may hold values from -0.125 to 0.125
- widening_matrices: bfloat16 [8, 2048, 1024], P('sp', None, 'tp'), may hold values from -0.125 to 0.125
- contracting_matrices: bfloat16 [8, 1024, 2048], P('sp', 'tp'), may hold values from -0.1875 to 0.1875
- assigned_specialist_ids: int32 [2048, 2], P(('grp', 'sp')), parts along dimension 0, may hold values from 0 to 7, as said below
- specialist_choice_affinity: float32 [2048, 2], P(('grp', 'sp', 'tp')), parts along dimension 0, may hold values from -6 to 6
- cluster_chance: float32 [2048], P(('grp', 'sp', 'tp')), parts along dimension 0, may hold values from 0.25 to 1
Outputs:
- layer_out: bfloat16 [2048, 2048], P(('grp', 'sp', 'tp')), parts along dimension 0
The draws below stay inside these ranges and needn't reach their ends.
There are 2 independent parts, one for each index of `grp`. The reference program is written for one: setup_inputs(seed, part) draws one part's arguments, and reference() takes and returns one part's arrays. A program takes and returns all parts, laid end to end along the dimension named above; an argument that names none is the same for every part. Nothing has to cross between parts.
Inputs may be any that keep to these rules, and one draw needn't show every extreme that they name: `assigned_specialist_ids`: each row names 2 different experts of one group: the experts g * 2 to (g + 1) * 2 - 1 for one g below 4. In each aligned block of 64 rows (the rows of one device) no expert is named by more than 32 rows, and every expert of one group, the same group in all blocks, is named by exactly 32 rows of every block. `channel_fading_rate`: positive.
All inputs are finite; a program needn't handle non-finite values.
Results may differ from the reference program's by a relative error of at most 0.015.
Values may be sent and summed in bfloat16 or wider, within the bound.
A program may use at most 64 MiB of HBM per device.

```python
import jax
import jax.numpy as jnp
from jax import lax

D = 2048
HEADS = 16
HEAD_DIM = 64
GROUPS_BC = 4
STATE = 128
CONV = 4
BLOCK = 64
FF = 1024
EGROUPS = 4
TOPK = 2
SEG_TOK = 256
D_SSD = 1024
ROWS = 64
TOKENS = 1024
EXPERTS = 8
CAP = 32
N_TP = 4


def draw_final_modulation_vector(key, part):
    row_key, column_key, base_key = jax.random.split(jax.random.fold_in(key, 7), 3)
    row_scale = jnp.exp(jax.random.uniform(row_key, (TOKENS, 1), jnp.float32, jnp.log(0.3), jnp.log(3.0)))
    column = jnp.arange(D_SSD, dtype=jnp.float32)[None, :] / D_SSD
    jitter = jnp.exp(jax.random.uniform(column_key, (1, D_SSD), jnp.float32, jnp.log(0.6), jnp.log(1.5)))
    base = jnp.clip(jax.random.normal(base_key, (TOKENS, D_SSD), jnp.float32), -4.0, 4.0)
    column_scale = jnp.exp(column * jnp.log(3.0)) * jitter
    return (base * row_scale * column_scale).astype(jnp.bfloat16)


def draw_raw_stride_amount(key, part):
    jitter_key, level_key = jax.random.split(jax.random.fold_in(key, 11))
    segments = TOKENS // SEG_TOK
    levels = jax.random.uniform(level_key, (segments, 1, 1), jnp.float32, -1.5, 1.0)
    jitter = jnp.clip(jax.random.normal(jitter_key, (segments, SEG_TOK, HEADS), jnp.float32), -4.5, 4.0)
    return (jitter + levels).reshape(TOKENS, HEADS)


def draw_channel_fading_rate(key, part):
    pick_key, slow_key, fast_key = jax.random.split(jax.random.fold_in(key, 13), 3)
    slow_share = 0.5
    is_slow = jax.random.uniform(pick_key, (HEADS,), jnp.float32) < slow_share
    slow_rates = jnp.exp(jax.random.uniform(slow_key, (HEADS,), jnp.float32, jnp.log(0.1 / TOKENS), jnp.log(1.0 / TOKENS)))
    fast_rates = jnp.exp(jax.random.uniform(fast_key, (HEADS,), jnp.float32, jnp.log(0.03), jnp.log(0.1)))
    return jnp.where(is_slow, slow_rates, fast_rates)


def draw_extra_log_attenuation(key, part):
    place_key, strength_key = jax.random.split(jax.random.fold_in(key, 17))
    places = jax.random.randint(place_key, (2, 1, HEADS), 0, TOKENS)
    strengths = jax.random.uniform(strength_key, (2, 1, HEADS), jnp.float32, 0.22, 0.69)
    positions = jnp.arange(TOKENS, dtype=jnp.int32)[None, :, None]
    return -jnp.sum(jnp.where(positions == places, strengths, 0.0), axis=0)


def draw_assigned_specialist_ids(key, part):
    blocks = TOKENS // ROWS
    per_group = EXPERTS // EGROUPS
    busy_rows = CAP * per_group // TOPK
    busy_key, other_key, order_key, deal_key = jax.random.split(jax.random.fold_in(key, 19), 4)
    busy_group = jax.random.randint(busy_key, (), 0, EGROUPS)
    others = jax.random.randint(other_key, (blocks, ROWS - busy_rows), 0, EGROUPS - 1)
    others = others + (others >= busy_group).astype(jnp.int32)
    groups = jnp.concatenate([jnp.full((blocks, busy_rows), busy_group, jnp.int32), others], axis=1)
    orders = jax.vmap(lambda subkey: jax.random.permutation(subkey, ROWS))(jax.random.split(order_key, blocks))
    groups = jnp.take_along_axis(groups, orders, axis=1)
    member = (groups[..., None] == jnp.arange(EGROUPS, dtype=jnp.int32)).astype(jnp.int32)
    ranking = jnp.sum((jnp.cumsum(member, axis=1) - member) * member, axis=2)
    dealing = jax.vmap(lambda subkey: jax.random.permutation(subkey, per_group))(jax.random.split(deal_key, blocks * EGROUPS)).reshape(blocks, EGROUPS, per_group)
    chosen = dealing[jnp.arange(blocks)[:, None], groups]
    first_place = TOPK * ranking % per_group
    first_pick = jnp.take_along_axis(chosen, first_place[..., None], axis=2)[..., 0]
    second_pick = jnp.take_along_axis(chosen, (first_place + 1)[..., None], axis=2)[..., 0]
    group_base = groups * per_group
    picked = jnp.stack([group_base + first_pick, group_base + second_pick], axis=-1)
    return picked.reshape(TOKENS, TOPK).astype(jnp.int32)


def block_levels(own_key, extent, cuts, low, top_value):
    def one(position, parts):
        steps = jax.random.uniform(jax.random.fold_in(jax.random.fold_in(own_key, 6), position), (parts,), jnp.float32, low / len(cuts), top_value / len(cuts))
        return jnp.repeat(jnp.exp(steps), extent[position] // parts).reshape((-1,) + (1,) * (len(extent) - position - 1))

    level = one(*cuts[0])
    for cut in cuts[1:]:
        level = level * one(*cut)
    return level


def centred(own_key, shape, width, limit, shards=(), kind=jnp.bfloat16):
    values = jax.random.normal(own_key, shape, jnp.float32) * width
    if len(shards) > 0:
        values = block_levels(own_key, shape, shards, -0.22, 0.18) * values
    return jnp.clip(values, min=-limit, max=limit).astype(kind)


def setup_inputs(seed: int = 0, part: int = 0) -> dict:
    streams_of = jax.random.split(jax.random.key(seed), 21)
    own_keys = jax.random.split(jax.random.fold_in(streams_of[20], part), 21)
    carryover_vector = centred(own_keys[0], (TOKENS, D), 1.0, 6.0, ((0, 16),))
    channel_source_entries = centred(own_keys[1], (TOKENS, D_SSD), 1.0, 6.0, ((0, 4), (1, 4)))
    final_modulation_vector = draw_final_modulation_vector(jax.random.fold_in(jax.random.fold_in(streams_of[20], part), 71), part)
    entering_basis_matrix = centred(own_keys[3], (TOKENS, GROUPS_BC * STATE), 1.0, 6.0, ((0, 4), (1, 4)))
    readout_basis_matrix = centred(own_keys[4], (TOKENS, GROUPS_BC * STATE), 1.0, 6.0, ((0, 4), (1, 4)))
    raw_stride_amount = draw_raw_stride_amount(jax.random.fold_in(jax.random.fold_in(streams_of[20], part), 71), part)
    extra_log_attenuation = draw_extra_log_attenuation(jax.random.fold_in(jax.random.fold_in(streams_of[20], part), 71), part)
    channel_fading_rate = draw_channel_fading_rate(jax.random.fold_in(streams_of[20], 71), part)
    channel_source_kernel = centred(streams_of[8], (CONV, D_SSD), CONV ** -0.5, 3.0, ((1, 4),), jnp.float32)
    entering_basis_kernel = centred(streams_of[9], (CONV, GROUPS_BC * STATE), CONV ** -0.5, 3.0, ((1, 4),), jnp.float32)
    readout_basis_kernel = centred(streams_of[10], (CONV, GROUPS_BC * STATE), CONV ** -0.5, 3.0, ((1, 4),), jnp.float32)
    modulated_rescaling_vector = jnp.clip(1.0 + 0.18 * jax.random.normal(streams_of[11], (D_SSD,), jnp.float32), 0.1, 1.9)
    blender_final_matrix = centred(streams_of[12], (D_SSD, D), D_SSD ** -0.5, 0.1875)
    specialist_rescaling_vector = jnp.clip(1.0 + 0.18 * jax.random.normal(streams_of[13], (D,), jnp.float32), 0.1, 1.9)
    specialist_gating_matrices = centred(streams_of[14], (EXPERTS, D, FF), D ** -0.5, 0.125, ((0, 4), (2, 4)))
    widening_matrices = centred(streams_of[15], (EXPERTS, D, FF), D ** -0.5, 0.125, ((0, 4), (2, 4)))
    contracting_matrices = centred(streams_of[16], (EXPERTS, FF, D), FF ** -0.5, 0.1875, ((0, 4), (1, 4)))
    assigned_specialist_ids = draw_assigned_specialist_ids(jax.random.fold_in(jax.random.fold_in(streams_of[20], part), 71), part)
    specialist_choice_affinity = centred(own_keys[18], (TOKENS, TOPK), 1.5, 6.0, ((0, 16),), jnp.float32)
    cluster_chance = jnp.clip(0.25 + 0.75 * jax.random.uniform(own_keys[19], (TOKENS,), jnp.float32) ** block_levels(own_keys[19], (TOKENS,), ((0, 16),), -0.2, 0.2), 0.25, 1.0)
    return dict(carryover_vector=carryover_vector, channel_source_entries=channel_source_entries, final_modulation_vector=final_modulation_vector, entering_basis_matrix=entering_basis_matrix, readout_basis_matrix=readout_basis_matrix, raw_stride_amount=raw_stride_amount, extra_log_attenuation=extra_log_attenuation, channel_fading_rate=channel_fading_rate, channel_source_kernel=channel_source_kernel, entering_basis_kernel=entering_basis_kernel, readout_basis_kernel=readout_basis_kernel, modulated_rescaling_vector=modulated_rescaling_vector, blender_final_matrix=blender_final_matrix, specialist_rescaling_vector=specialist_rescaling_vector, specialist_gating_matrices=specialist_gating_matrices, widening_matrices=widening_matrices, contracting_matrices=contracting_matrices, assigned_specialist_ids=assigned_specialist_ids, specialist_choice_affinity=specialist_choice_affinity, cluster_chance=cluster_chance)


EPS = 1e-06
HIGHEST = lax.Precision.HIGHEST

def causal_conv(signal, weights):
    kernel_len = weights.shape[0]
    length = signal.shape[0]
    padded = jnp.pad(signal.astype(jnp.float32), ((kernel_len - 1, 0), (0, 0)))
    accumulated = jnp.zeros((length, signal.shape[1]), jnp.float32)
    for offset in range(kernel_len):
        accumulated = accumulated + weights[offset][None, :] * padded[offset:offset + length]
    return jax.nn.silu(accumulated)

def state_space(scaled_in, log_attenuation, keys_b, queries_c):
    blocks = scaled_in.shape[0] // BLOCK
    per_group = HEADS // GROUPS_BC
    scaled_in = scaled_in.reshape(blocks, BLOCK, GROUPS_BC, per_group, HEAD_DIM)
    log_attenuation = log_attenuation.reshape(blocks, BLOCK, GROUPS_BC, per_group)
    keys_b = keys_b.reshape(blocks, BLOCK, GROUPS_BC, STATE)
    queries_c = queries_c.reshape(blocks, BLOCK, GROUPS_BC, STATE)
    lower_mask = jnp.tril(jnp.ones((BLOCK, BLOCK), dtype=bool))

    def advance(carried, pieces):
        block_in, block_log, block_b, block_c = pieces
        running = jnp.cumsum(block_log, axis=0)
        between = running[:, None] - running[None, :]
        decays = jnp.exp(jnp.where(lower_mask[:, :, None, None], between, -jnp.inf))
        scores = jnp.einsum('lgn,sgn->lsg', block_c, block_b, precision=HIGHEST)
        inside = jnp.einsum('lsg,lsgr,sgrp->lgrp', scores, decays, block_in, precision=HIGHEST)
        outside = jnp.einsum('lgn,grpn,lgr->lgrp', block_c, carried, jnp.exp(running), precision=HIGHEST)
        remain = jnp.exp(running[-1][None] - running)
        updated = carried * jnp.exp(running[-1])[:, :, None, None] + jnp.einsum('sgn,sgr,sgrp->grpn', block_b, remain, block_in, precision=HIGHEST)
        return (updated, inside + outside)
    initial = jnp.zeros((GROUPS_BC, per_group, HEAD_DIM, STATE), jnp.float32)
    _, outputs = lax.scan(advance, initial, (scaled_in, log_attenuation, keys_b, queries_c))
    return outputs.reshape(blocks * BLOCK, HEADS, HEAD_DIM)

def reference(carryover_vector, channel_source_entries, final_modulation_vector, entering_basis_matrix, readout_basis_matrix, raw_stride_amount, extra_log_attenuation, channel_fading_rate, channel_source_kernel, entering_basis_kernel, readout_basis_kernel, modulated_rescaling_vector, blender_final_matrix, specialist_rescaling_vector, specialist_gating_matrices, widening_matrices, contracting_matrices, assigned_specialist_ids, specialist_choice_affinity, cluster_chance):
    length = carryover_vector.shape[0]
    inputs_x = causal_conv(channel_source_entries, channel_source_kernel)
    keys_b = causal_conv(entering_basis_matrix, entering_basis_kernel)
    queries_c = causal_conv(readout_basis_matrix, readout_basis_kernel)
    channel_stride_amount = jax.nn.softplus(raw_stride_amount)
    log_attenuation = extra_log_attenuation - channel_fading_rate[None, :] * channel_stride_amount
    heads_x = inputs_x.reshape(length, HEADS, HEAD_DIM)
    mixed = state_space(heads_x * channel_stride_amount[:, :, None], log_attenuation, keys_b, queries_c)
    gated = mixed.reshape(length, D_SSD) * jax.nn.silu(final_modulation_vector.astype(jnp.float32))
    normed = (gated * lax.rsqrt(lax.optimization_barrier(jnp.mean(gated * gated, axis=1, keepdims=True)) + EPS) * modulated_rescaling_vector[None, :]).astype(jnp.bfloat16)
    middle = (carryover_vector.astype(jnp.float32) + jnp.dot(normed, blender_final_matrix, preferred_element_type=jnp.float32)).astype(jnp.bfloat16)
    middle_wide = middle.astype(jnp.float32)
    expert_input = (middle_wide * lax.rsqrt(lax.optimization_barrier(jnp.mean(middle_wide * middle_wide, axis=1, keepdims=True)) + EPS) * specialist_rescaling_vector[None, :]).astype(jnp.bfloat16)
    assigned = assigned_specialist_ids.reshape(-1)
    count_all = assigned.shape[0]
    member = (assigned[:, None] == jnp.arange(EXPERTS, dtype=jnp.int32)[None, :]).astype(jnp.int32)
    ranking = lax.optimization_barrier(jnp.sum((jnp.cumsum(member, axis=0) - member) * member, axis=1))
    slot_count = length // ROWS * CAP
    table = jnp.full((EXPERTS, slot_count), -1, jnp.int32).at[assigned, ranking].set(jnp.arange(count_all, dtype=jnp.int32))
    lifted = jnp.exp(specialist_choice_affinity)
    shares = (cluster_chance[:, None] * lifted / lax.optimization_barrier(jnp.sum(lifted, axis=1, keepdims=True))).reshape(-1)
    quarter = FF // N_TP

    def expert_pass(combined, expert_index):
        slot_ids = table[expert_index]
        is_live = slot_ids >= 0
        safe_ids = jnp.maximum(slot_ids, 0)
        token_ids = safe_ids // TOPK
        chosen = jnp.take(expert_input, token_ids, axis=0)
        gate_value = jnp.dot(chosen, specialist_gating_matrices[expert_index], preferred_element_type=jnp.float32)
        up_value = jnp.dot(chosen, widening_matrices[expert_index], preferred_element_type=jnp.float32)
        hidden = (jax.nn.silu(gate_value) * up_value).astype(jnp.bfloat16)
        down_rows = contracting_matrices[expert_index]
        summed = jnp.zeros((slot_count, D), jnp.float32)
        for part_index in range(N_TP):
            piece_sum = jnp.dot(hidden[:, part_index * quarter:(part_index + 1) * quarter], down_rows[part_index * quarter:(part_index + 1) * quarter], preferred_element_type=jnp.float32).astype(jnp.bfloat16)
            summed = summed + lax.optimization_barrier(piece_sum).astype(jnp.float32)
        result = lax.optimization_barrier(summed.astype(jnp.bfloat16)).astype(jnp.float32)
        weight_column = jnp.where(is_live, shares[safe_ids], 0.0)
        return (combined.at[token_ids].add(weight_column[:, None] * result), None)
    combined, _ = lax.scan(expert_pass, jnp.zeros((length, D), jnp.float32), jnp.arange(EXPERTS, dtype=jnp.int32))
    return (middle_wide + combined).astype(jnp.bfloat16)
```

```python
import functools

import jax
import jax.numpy as jnp
from jax import lax
from jax.experimental import pallas as pl
from jax.experimental.pallas import tpu as pltpu
from jax.sharding import PartitionSpec as P

HEAD_DIM = 64
STATE = 128
EXPERT_GROUPS = 4
EPS = 1e-06
HIGHEST = lax.Precision.HIGHEST
F32 = jnp.float32
BF16 = jnp.bfloat16
TAIL = 16


def silu(v):
    return v / (1.0 + jnp.exp(-v))


def first_dims(a, b, precision=None):
    return lax.dot_general(
        a, b, (((0,), (0,)), ((), ())), precision=precision, preferred_element_type=F32
    )


def spread(cols, width):
    heads = cols.shape[1]
    lane_head = lax.broadcasted_iota(jnp.int32, (cols.shape[0], width), 1) // HEAD_DIM
    out = jnp.broadcast_to(cols[:, 0:1], (cols.shape[0], width))
    for h in range(1, heads):
        out = jnp.where(lane_head == h, cols[:, h : h + 1], out)
    return out


def routing(meta, first_expert, rows, cap, locals_):
    id0, id1 = meta[0:1, :rows], meta[1:2, :rows]
    hit0 = (id0 >= first_expert) & (id0 < first_expert + locals_)
    hit1 = (id1 >= first_expert) & (id1 < first_expert + locals_)
    hit = jnp.where(hit0 | hit1, 1.0, 0.0)
    earlier = lax.broadcasted_iota(jnp.int32, (rows, rows), 0) < lax.broadcasted_iota(
        jnp.int32, (rows, rows), 1
    )
    place = jnp.dot(
        jnp.broadcast_to(hit, (8, rows)).astype(BF16),
        jnp.where(earlier, 1.0, 0.0).astype(BF16),
        preferred_element_type=F32,
    )[0:1]
    slot = lax.broadcasted_iota(jnp.int32, (cap, rows), 0).astype(F32)
    return jnp.where((place == slot) & (hit > 0.5), 1.0, 0.0)


def kernel(
    n,
    tp,
    cap,
    x_ref,
    b_ref,
    c_ref,
    z_ref,
    raw_ref,
    extra_ref,
    fade_ref,
    kx_ref,
    kb_ref,
    kc_ref,
    gain_ref,
    blend_hbm,
    sgain_ref,
    wg_hbm,
    wu_hbm,
    wd_hbm,
    meta_ref,
    carry_ref,
    out_ref,
    blend,
    wg,
    wu,
    wd,
    tail_x,
    tail_b,
    tail_c,
    ext,
    st_send,
    tot_send,
    st_buf,
    tot_buf,
    g_send,
    g_buf,
    mid,
    metas,
    x_send,
    arr,
    part,
    rs1,
    far_send,
    rs2,
    ret_send,
    ret,
    local_sem,
    tail_ss,
    tail_rs,
    st_ss,
    st_rs,
    tot_ss,
    tot_rs,
    meta_ss,
    meta_rs,
    g_ss,
    g_rs,
    z_ss,
    z_rs,
    far_ss,
    far_rs,
    near_ss,
    near_rs,
    p1_ss,
    p1_rs,
    p2_ss,
    p2_rs,
    ret_ss,
    ret_rs,
):
    s = lax.axis_index("sp")
    t = lax.axis_index("tp")
    length, width = x_ref.shape
    rows, model = carry_ref.shape
    heads = width // HEAD_DIM
    locals_ = wg_hbm.shape[0]
    far = (t + tp // 2) % tp
    near = t + 1 - 2 * (t % 2)
    near_far = (near + tp // 2) % tp

    def remote(src, dst, ssem, rsem, sp, tpi):
        return pltpu.make_async_remote_copy(
            src_ref=src,
            dst_ref=dst,
            send_sem=ssem,
            recv_sem=rsem,
            device_id={"sp": sp, "tp": tpi},
            device_id_type=pl.DeviceIdType.MESH,
        )

    barrier = pltpu.get_barrier_semaphore()
    for k in range(n):
        for q in range(tp):
            if k or q:
                pl.semaphore_signal(
                    barrier,
                    inc=1,
                    device_id={"sp": (s + k) % n, "tp": (t + q) % tp},
                    device_id_type=pl.DeviceIdType.MESH,
                )
    fetches = [
        pltpu.make_async_copy(src, dst, local_sem.at[i])
        for i, (src, dst) in enumerate(
            ((blend_hbm, blend), (wg_hbm, wg), (wu_hbm, wu), (wd_hbm, wd))
        )
    ]
    for fetch in fetches:
        fetch.start()

    dt = jnp.log1p(jnp.exp(raw_ref[...]))
    la = extra_ref[...] - fade_ref[...] * dt
    row_i = lax.broadcasted_iota(jnp.int32, (length, length), 0)
    col_i = lax.broadcasted_iota(jnp.int32, (length, length), 1)
    lower = row_i >= col_i
    cum = jnp.dot(
        jnp.where(lower, 1.0, 0.0), la, precision=HIGHEST, preferred_element_type=F32
    )
    cum_t = first_dims(la, jnp.where(row_i <= col_i, 1.0, 0.0), HIGHEST)

    pl.semaphore_wait(barrier, n * tp - 1)

    sends = []
    following = (s + 1) % n
    tails = []
    for i, (src, dst) in enumerate(((x_ref, tail_x), (b_ref, tail_b), (c_ref, tail_c))):
        copy = remote(
            src.at[pl.ds(length - TAIL, TAIL)], dst, tail_ss.at[i], tail_rs.at[i], following, t
        )
        copy.start()
        tails.append(copy)
    meta_copies = []
    for k in range(n):
        for q in range(tp):
            if k or q:
                copy = remote(
                    meta_ref,
                    metas.at[k, q],
                    meta_ss.at[k, q],
                    meta_rs.at[k, q],
                    (s + k) % n,
                    (t + q) % tp,
                )
                copy.start()
                meta_copies.append(copy)
    metas[0, 0] = meta_ref[...]

    ext[TAIL:, 0:width] = x_ref[...].astype(F32)
    ext[TAIL:, width : width + STATE] = b_ref[...].astype(F32)
    ext[TAIL:, width + STATE : width + 2 * STATE] = c_ref[...].astype(F32)
    for copy in tails:
        copy.wait()
    inner = s > 0
    ext[0:TAIL, 0:width] = jnp.where(inner, tail_x[...].astype(F32), 0.0)
    ext[0:TAIL, width : width + STATE] = jnp.where(inner, tail_b[...].astype(F32), 0.0)
    ext[0:TAIL, width + STATE : width + 2 * STATE] = jnp.where(
        inner, tail_c[...].astype(F32), 0.0
    )

    def conv(taps, first, count):
        kernel_len = taps.shape[0]
        total = None
        for j in range(kernel_len):
            at = TAIL - kernel_len + 1 + j
            term = taps[j : j + 1, :] * ext[at : at + length, first : first + count]
            total = term if total is None else total + term
        return silu(total)

    keys = conv(kb_ref, width, STATE).astype(BF16)
    xdt = conv(kx_ref, 0, width) * spread(dt, width)
    tot = cum[length - 1 : length, :]
    remain = jnp.exp(tot - cum)
    state = first_dims(keys, (xdt * spread(remain, width)).astype(BF16))
    st_send[...] = state.astype(BF16)
    tot_send[...] = jnp.broadcast_to(spread(tot, width), tot_send.shape)
    states = []
    for k in range(1, n):
        a = remote(st_send, st_buf.at[k], st_ss.at[k], st_rs.at[k], (s + k) % n, t)
        b = remote(tot_send, tot_buf.at[k], tot_ss.at[k], tot_rs.at[k], (s + k) % n, t)
        b.start()
        a.start()
        states += [a, b]

    queries = conv(kc_ref, width + STATE, STATE).astype(BF16)
    scores = lax.dot_general(
        queries, keys, (((1,), (1,)), ((), ())), preferred_element_type=F32
    )
    xdt_b = xdt.astype(BF16)
    lane_head = lax.broadcasted_iota(jnp.int32, (length, width), 1) // HEAD_DIM
    mixed = jnp.zeros((length, width), F32)
    for h in range(heads):
        between = jnp.where(lower, cum[:, h : h + 1] - cum_t[h : h + 1, :], -1e30)
        weights = (scores * jnp.exp(between)).astype(BF16)
        chosen = jnp.where(lane_head == h, xdt_b, jnp.zeros_like(xdt_b))
        mixed = mixed + jnp.dot(weights, chosen, preferred_element_type=F32)
    reach = jnp.exp(spread(cum, width))
    modulation = silu(z_ref[...].astype(F32))

    for copy in states:
        copy.wait()
    incoming = jnp.zeros((STATE, width), F32)
    for k in range(n - 1, 0, -1):
        later = incoming * jnp.exp(tot_buf[k, 0:1, :]) + st_buf[k].astype(F32)
        incoming = jnp.where(k <= s, later, incoming)
    outside = jnp.dot(queries, incoming.astype(BF16), preferred_element_type=F32)
    g_send[...] = ((mixed + outside * reach) * modulation).astype(BF16)
    spreads = []
    for q in (2, 3, 1) if tp == 4 else range(1, tp):
        to = (t + q) % tp
        copy = remote(
            g_send.at[pl.ds(to * rows, rows)], g_buf.at[t], g_ss.at[q], g_rs.at[q], s, to
        )
        copy.start()
        spreads.append(copy)
    g_buf[t] = g_send[pl.ds(pl.multiple_of(t * rows, rows), rows), :]

    own_meta = meta_ref[...]
    onehots = []
    for k in range(n):
        first = ((s + k) % n * locals_).astype(F32)
        onehots.append(routing(own_meta, first, rows, cap, locals_).astype(BF16))
    for copy in meta_copies:
        copy.wait()
    fetches[0].wait()
    for copy in spreads:
        copy.wait()
    squares = jnp.zeros((rows, 1), F32)
    for i in range(tp):
        piece = g_buf[i].astype(F32)
        squares = squares + jnp.sum(piece * piece, axis=1, keepdims=True)
    scale = lax.rsqrt(squares / (tp * width) + EPS)
    projected = carry_ref[...].astype(F32)
    for i in range(tp):
        span = slice(i * width, (i + 1) * width)
        normed = (g_buf[i].astype(F32) * scale * gain_ref[:, span]).astype(BF16)
        projected = projected + jnp.dot(normed, blend[span, :], preferred_element_type=F32)
    middle = projected.astype(BF16)
    mid[...] = middle
    wide = middle.astype(F32)
    expert_in = (
        wide
        * lax.rsqrt(jnp.mean(wide * wide, axis=1, keepdims=True) + EPS)
        * sgain_ref[...]
    ).astype(BF16)

    order = []
    for k in range(n // 2 + 1):
        for other in (k, (n - k) % n):
            if other not in order:
                order.append(other)

    z_copies, far_copies, near_copies, p1_copies, p2_copies, ret_copies = {}, {}, {}, {}, {}, {}
    for k in order[1:] + order[:1]:
        picked = jnp.dot(onehots[k], expert_in, preferred_element_type=F32).astype(BF16)
        if k == 0:
            arr[0, t] = picked
        else:
            x_send[k] = picked
            z_copies[k] = remote(
                x_send.at[k], arr.at[k, t], z_ss.at[k], z_rs.at[k], (s + k) % n, t
            )
            z_copies[k].start()

    def pass_far(k):
        if k:
            z_copies[k].wait()
        far_copies[k] = remote(arr.at[k, t], arr.at[k, t], far_ss.at[k], far_rs.at[k], s, far)
        far_copies[k].start()
        first = remote(
            arr.at[k, t], arr.at[k, t], near_ss.at[k, 0], near_rs.at[k, 0], s, near
        )
        first.start()
        near_copies[k] = [first]

    def pass_near(k):
        far_copies[k].wait()
        second = remote(
            arr.at[k, far], arr.at[k, far], near_ss.at[k, 1], near_rs.at[k, 1], s, near
        )
        second.start()
        near_copies[k].append(second)

    weight_row0 = s * locals_

    def slot_weights(k):
        columns = [[] for _ in range(locals_)]
        for i in range(tp):
            q = (t + tp - i) % tp
            meta = metas[k, q]
            onehot = routing(meta, weight_row0.astype(F32), rows, cap, locals_)
            for l in range(locals_):
                expert = (weight_row0 + l).astype(F32)
                lift0, lift1 = jnp.exp(meta[2:3, :rows]), jnp.exp(meta[3:4, :rows])
                share = meta[4:5, :rows] / (lift0 + lift1)
                mine = share * (
                    jnp.where(meta[0:1, :rows] == expert, lift0, 0.0)
                    + jnp.where(meta[1:2, :rows] == expert, lift1, 0.0)
                )
                columns[l].append(jnp.sum(onehot * mine, axis=1, keepdims=True))
        return [jnp.concatenate(c, axis=0) for c in columns]

    def experts(k):
        shares = slot_weights(k)
        for copy in near_copies[k]:
            copy.wait()
        tokens = arr[k].reshape(tp * cap, model)
        if not loaded:
            for fetch in fetches[1:]:
                fetch.wait()
            loaded.append(True)
        total = None
        for l in range(locals_):
            gate = jnp.dot(tokens, wg[l], preferred_element_type=F32)
            up = jnp.dot(tokens, wu[l], preferred_element_type=F32)
            hidden = (silu(gate) * up * shares[l]).astype(BF16)
            term = jnp.dot(hidden, wd[l], preferred_element_type=F32)
            total = term if total is None else total + term
        part[k] = total.astype(BF16).reshape(tp, cap, model)
        pair = []
        for i, owner in ((1, near_far), (0, near)):
            copy = remote(
                part.at[k, owner], rs1.at[k, i], p1_ss.at[k, i], p1_rs.at[k, i], s, near
            )
            copy.start()
            pair.append(copy)
        p1_copies[k] = pair

    def reduce_near(k):
        for copy in p1_copies[k]:
            copy.wait()
        far_send[k] = (part[k, far].astype(F32) + rs1[k, 1].astype(F32)).astype(BF16)
        p2_copies[k] = remote(far_send.at[k], rs2.at[k], p2_ss.at[k], p2_rs.at[k], s, far)
        p2_copies[k].start()

    def reduce_far(k):
        p2_copies[k].wait()
        total = (
            part[k, t].astype(F32) + rs1[k, 0].astype(F32) + rs2[k].astype(F32)
        ).astype(BF16)
        if k == 0:
            ret[0] = total
        else:
            ret_send[k] = total
            ret_copies[k] = remote(
                ret_send.at[k], ret.at[k], ret_ss.at[k], ret_rs.at[k], (s + n - k) % n, t
            )
            ret_copies[k].start()

    loaded = []
    pass_far(order[0])
    for i in range(n + 2):
        if i + 1 < n:
            pass_far(order[i + 1])
        if i < n:
            pass_near(order[i])
            experts(order[i])
        if 0 <= i - 1 < n:
            reduce_near(order[i - 1])
        if 0 <= i - 2 < n:
            reduce_far(order[i - 2])

    result = mid[...].astype(F32)
    for k in order:
        if k:
            ret_copies[k].wait()
        result = result + first_dims(onehots[k], ret[k])
    out_ref[...] = result.astype(BF16)


def per_device(
    n,
    tp,
    carryover_vector,
    channel_source_entries,
    final_modulation_vector,
    entering_basis_matrix,
    readout_basis_matrix,
    raw_stride_amount,
    extra_log_attenuation,
    channel_fading_rate,
    channel_source_kernel,
    entering_basis_kernel,
    readout_basis_kernel,
    modulated_rescaling_vector,
    blender_final_matrix,
    specialist_rescaling_vector,
    specialist_gating_matrices,
    widening_matrices,
    contracting_matrices,
    assigned_specialist_ids,
    specialist_choice_affinity,
    cluster_chance,
):
    length, width = channel_source_entries.shape
    rows, model = carryover_vector.shape
    locals_, _, hidden = specialist_gating_matrices.shape
    experts = n * locals_
    picks = assigned_specialist_ids.shape[1]
    assert tp == 4 and picks == 2 and entering_basis_matrix.shape[1] == STATE
    per_expert = 2 * rows * picks // experts
    group_size = experts // EXPERT_GROUPS
    if group_size <= locals_:
        cap = locals_ * per_expert // picks
    else:
        cap = locals_ * per_expert
    cap = -(-min(cap, rows) // 16) * 16
    own_ids = lax.dynamic_slice_in_dim(
        assigned_specialist_ids, lax.axis_index("tp") * rows, rows, 0
    )
    meta = jnp.concatenate(
        [
            own_ids.astype(F32),
            specialist_choice_affinity,
            cluster_chance[:, None],
            jnp.zeros((rows, 3), F32),
        ],
        axis=1,
    ).T
    meta = jnp.pad(meta, ((0, 0), (0, 128 - rows)))
    vmem = pl.BlockSpec(memory_space=pltpu.VMEM)
    hbm = pl.BlockSpec(memory_space=pl.ANY)
    dma = pltpu.SemaphoreType.DMA
    scratch = [
        pltpu.VMEM(blender_final_matrix.shape, BF16),
        pltpu.VMEM(specialist_gating_matrices.shape, BF16),
        pltpu.VMEM(widening_matrices.shape, BF16),
        pltpu.VMEM(contracting_matrices.shape, BF16),
        pltpu.VMEM((TAIL, width), BF16),
        pltpu.VMEM((TAIL, STATE), BF16),
        pltpu.VMEM((TAIL, STATE), BF16),
        pltpu.VMEM((TAIL + length, width + 2 * STATE), F32),
        pltpu.VMEM((STATE, width), BF16),
        pltpu.VMEM((8, width), F32),
        pltpu.VMEM((n, STATE, width), BF16),
        pltpu.VMEM((n, 8, width), F32),
        pltpu.VMEM((length, width), BF16),
        pltpu.VMEM((tp, rows, width), BF16),
        pltpu.VMEM((rows, model), BF16),
        pltpu.VMEM((n, tp, 8, 128), F32),
        pltpu.VMEM((n, cap, model), BF16),
        pltpu.VMEM((n, tp, cap, model), BF16),
        pltpu.VMEM((n, tp, cap, model), BF16),
        pltpu.VMEM((n, 2, cap, model), BF16),
        pltpu.VMEM((n, cap, model), BF16),
        pltpu.VMEM((n, cap, model), BF16),
        pltpu.VMEM((n, cap, model), BF16),
        pltpu.VMEM((n, cap, model), BF16),
        dma((4,)),
    ]
    for shape in ((3,), (n,), (n,), (n, tp), (tp,), (n,), (n,), (n, 2), (n, 2), (n,), (n,)):
        scratch += [dma(shape), dma(shape)]
    return pl.pallas_call(
        functools.partial(kernel, n, tp, cap),
        out_shape=jax.ShapeDtypeStruct((rows, model), BF16),
        in_specs=[vmem] * 11 + [hbm, vmem, hbm, hbm, hbm, vmem, vmem],
        out_specs=vmem,
        scratch_shapes=scratch,
        compiler_params=pltpu.CompilerParams(
            collective_id=0, has_side_effects=True, vmem_limit_bytes=60 * 1024 * 1024
        ),
    )(
        channel_source_entries,
        entering_basis_matrix,
        readout_basis_matrix,
        final_modulation_vector,
        raw_stride_amount,
        extra_log_attenuation,
        channel_fading_rate[None, :],
        channel_source_kernel,
        entering_basis_kernel,
        readout_basis_kernel,
        modulated_rescaling_vector[None, :],
        blender_final_matrix,
        specialist_rescaling_vector[None, :],
        specialist_gating_matrices,
        widening_matrices,
        contracting_matrices,
        meta,
        carryover_vector,
    )


def solution(mesh):
    return jax.shard_map(
        functools.partial(per_device, mesh.shape["sp"], mesh.shape["tp"]),
        mesh=mesh,
        in_specs=(
            P(("grp", "sp", "tp"), None),
            P(("grp", "sp"), "tp"),
            P(("grp", "sp"), "tp"),
            P(("grp", "sp"), "tp"),
            P(("grp", "sp"), "tp"),
            P(("grp", "sp"), "tp"),
            P(("grp", "sp"), "tp"),
            P("tp"),
            P(None, "tp"),
            P(None, "tp"),
            P(None, "tp"),
            P(),
            P(),
            P(),
            P("sp", None, "tp"),
            P("sp", None, "tp"),
            P("sp", "tp", None),
            P(("grp", "sp"), None),
            P(("grp", "sp", "tp"), None),
            P(("grp", "sp", "tp")),
        ),
        out_specs=P(("grp", "sp", "tp"), None),
        check_vma=False,
    )
```

```python
import functools

import jax
import jax.numpy as jnp
from jax import lax
from jax.experimental import pallas as pl
from jax.experimental.pallas import tpu as pltpu
from jax.sharding import PartitionSpec as P

HEAD_DIM = 64
STATE = 128
EXPERT_GROUPS = 4
EPS = 1e-06
HIGHEST = lax.Precision.HIGHEST
F32 = jnp.float32
BF16 = jnp.bfloat16
TAIL = 16


def silu(v):
    return v / (1.0 + jnp.exp(-v))


def first_dims(a, b, precision=None):
    return lax.dot_general(
        a, b, (((0,), (0,)), ((), ())), precision=precision, preferred_element_type=F32
    )


def last_dims(a, b):
    return lax.dot_general(
        a, b, (((1,), (1,)), ((), ())), precision=HIGHEST, preferred_element_type=F32
    )


def spread(cols, width):
    heads = cols.shape[1]
    lane_head = lax.broadcasted_iota(jnp.int32, (cols.shape[0], width), 1) // HEAD_DIM
    out = jnp.broadcast_to(cols[:, 0:1], (cols.shape[0], width))
    for h in range(1, heads):
        out = jnp.where(lane_head == h, cols[:, h : h + 1], out)
    return out


def routing(meta, first_expert, rows, cap, locals_):
    id0, id1 = meta[0:1, :rows], meta[1:2, :rows]
    hit0 = (id0 >= first_expert) & (id0 < first_expert + locals_)
    hit1 = (id1 >= first_expert) & (id1 < first_expert + locals_)
    hit = jnp.where(hit0 | hit1, 1.0, 0.0)
    earlier = lax.broadcasted_iota(jnp.int32, (rows, rows), 0) < lax.broadcasted_iota(
        jnp.int32, (rows, rows), 1
    )
    place = jnp.dot(
        jnp.broadcast_to(hit, (8, rows)).astype(BF16),
        jnp.where(earlier, 1.0, 0.0).astype(BF16),
        preferred_element_type=F32,
    )[0:1]
    slot = lax.broadcasted_iota(jnp.int32, (cap, rows), 0).astype(F32)
    return jnp.where((place == slot) & (hit > 0.5), 1.0, 0.0)


def kernel(
    n,
    tp,
    cap,
    x_ref,
    b_ref,
    c_ref,
    z_ref,
    raw_ref,
    extra_ref,
    fade_ref,
    kx_ref,
    kb_ref,
    kc_ref,
    gain_ref,
    blend_hbm,
    sgain_ref,
    wg_hbm,
    wu_hbm,
    wd_hbm,
    ids_ref,
    aff_ref,
    chance_ref,
    carry_ref,
    out_ref,
    blend,
    wg,
    wu,
    wd,
    tail_x,
    tail_b,
    tail_c,
    ext,
    st_send,
    tot_send,
    st_buf,
    tot_buf,
    g_send,
    g_buf,
    mid,
    meta_ref,
    metas,
    x_send,
    arr,
    part,
    rs1,
    far_send,
    rs2,
    ret_send,
    ret,
    local_sem,
    tail_ss,
    tail_rs,
    st_ss,
    st_rs,
    tot_ss,
    tot_rs,
    meta_ss,
    meta_rs,
    g_ss,
    g_rs,
    z_ss,
    z_rs,
    far_ss,
    far_rs,
    near_ss,
    near_rs,
    p1_ss,
    p1_rs,
    p2_ss,
    p2_rs,
    ret_ss,
    ret_rs,
):
    s = lax.axis_index("sp")
    t = lax.axis_index("tp")
    length, width = x_ref.shape
    rows, model = carry_ref.shape
    heads = width // HEAD_DIM
    locals_ = wg_hbm.shape[0]
    far = (t + tp // 2) % tp
    near = t + 1 - 2 * (t % 2)
    near_far = (near + tp // 2) % tp

    def remote(src, dst, ssem, rsem, sp, tpi):
        return pltpu.make_async_remote_copy(
            src_ref=src,
            dst_ref=dst,
            send_sem=ssem,
            recv_sem=rsem,
            device_id={"sp": sp, "tp": tpi},
            device_id_type=pl.DeviceIdType.MESH,
        )

    barrier = pltpu.get_barrier_semaphore()
    for k in range(n):
        for q in range(tp):
            if k or q:
                pl.semaphore_signal(
                    barrier,
                    inc=1,
                    device_id={"sp": (s + k) % n, "tp": (t + q) % tp},
                    device_id_type=pl.DeviceIdType.MESH,
                )
    fetches = [
        pltpu.make_async_copy(src, dst, local_sem.at[i])
        for i, (src, dst) in enumerate(
            ((blend_hbm, blend), (wg_hbm, wg), (wu_hbm, wu), (wd_hbm, wd))
        )
    ]
    for fetch in fetches:
        fetch.start()

    dt_t = jnp.log1p(jnp.exp(raw_ref[...]))
    la_t = extra_ref[...] - fade_ref[...] * dt_t
    row_i = lax.broadcasted_iota(jnp.int32, (length, length), 0)
    col_i = lax.broadcasted_iota(jnp.int32, (length, length), 1)
    lower = row_i >= col_i
    cum = last_dims(jnp.where(lower, 1.0, 0.0), la_t)
    dt = last_dims(jnp.where(row_i == col_i, 1.0, 0.0), dt_t)
    cum_t = jnp.dot(
        la_t,
        jnp.where(row_i <= col_i, 1.0, 0.0),
        precision=HIGHEST,
        preferred_element_type=F32,
    )
    meta_ref[...] = jnp.zeros_like(meta_ref)
    ids = ids_ref[:, 0:rows]
    for i in range(1, tp):
        ids = jnp.where(t == i, ids_ref[:, i * rows : (i + 1) * rows], ids)
    meta_ref[0:2, 0:rows] = ids.astype(F32)
    meta_ref[2:4, 0:rows] = aff_ref[...]
    meta_ref[4:5, 0:rows] = chance_ref[...]

    pl.semaphore_wait(barrier, n * tp - 1)

    sends = []
    following = (s + 1) % n
    tails = []
    for i, (src, dst) in enumerate(((x_ref, tail_x), (b_ref, tail_b), (c_ref, tail_c))):
        copy = remote(
            src.at[pl.ds(length - TAIL, TAIL)], dst, tail_ss.at[i], tail_rs.at[i], following, t
        )
        copy.start()
        tails.append(copy)
    meta_copies = []
    for k in range(n):
        for q in range(tp):
            if k or q:
                copy = remote(
                    meta_ref,
                    metas.at[k, q],
                    meta_ss.at[k, q],
                    meta_rs.at[k, q],
                    (s + k) % n,
                    (t + q) % tp,
                )
                copy.start()
                meta_copies.append(copy)
    metas[0, 0] = meta_ref[...]

    ext[TAIL:, 0:width] = x_ref[...].astype(F32)
    ext[TAIL:, width : width + STATE] = b_ref[...].astype(F32)
    ext[TAIL:, width + STATE : width + 2 * STATE] = c_ref[...].astype(F32)
    for copy in tails:
        copy.wait()
    inner = s > 0
    ext[0:TAIL, 0:width] = jnp.where(inner, tail_x[...].astype(F32), 0.0)
    ext[0:TAIL, width : width + STATE] = jnp.where(inner, tail_b[...].astype(F32), 0.0)
    ext[0:TAIL, width + STATE : width + 2 * STATE] = jnp.where(
        inner, tail_c[...].astype(F32), 0.0
    )

    def conv(taps, first, count):
        kernel_len = taps.shape[0]
        total = None
        for j in range(kernel_len):
            at = TAIL - kernel_len + 1 + j
            term = taps[j : j + 1, :] * ext[at : at + length, first : first + count]
            total = term if total is None else total + term
        return silu(total)

    keys = conv(kb_ref, width, STATE).astype(BF16)
    xdt = conv(kx_ref, 0, width) * spread(dt, width)
    tot = cum[length - 1 : length, :]
    remain = jnp.exp(tot - cum)
    state = first_dims(keys, (xdt * spread(remain, width)).astype(BF16))
    st_send[...] = state.astype(BF16)
    tot_send[...] = jnp.broadcast_to(spread(tot, width), tot_send.shape)
    states = []
    for k in range(1, n):
        a = remote(st_send, st_buf.at[k], st_ss.at[k], st_rs.at[k], (s + k) % n, t)
        b = remote(tot_send, tot_buf.at[k], tot_ss.at[k], tot_rs.at[k], (s + k) % n, t)
        b.start()
        a.start()
        states += [a, b]

    queries = conv(kc_ref, width + STATE, STATE).astype(BF16)
    scores = lax.dot_general(
        queries, keys, (((1,), (1,)), ((), ())), preferred_element_type=F32
    )
    xdt_b = xdt.astype(BF16)
    lane_head = lax.broadcasted_iota(jnp.int32, (length, width), 1) // HEAD_DIM
    mixed = jnp.zeros((length, width), F32)
    for h in range(heads):
        between = jnp.where(lower, cum[:, h : h + 1] - cum_t[h : h + 1, :], -1e30)
        weights = (scores * jnp.exp(between)).astype(BF16)
        chosen = jnp.where(lane_head == h, xdt_b, jnp.zeros_like(xdt_b))
        mixed = mixed + jnp.dot(weights, chosen, preferred_element_type=F32)
    reach = jnp.exp(spread(cum, width))
    modulation = silu(z_ref[...].astype(F32))

    for copy in states:
        copy.wait()
    incoming = jnp.zeros((STATE, width), F32)
    for k in range(n - 1, 0, -1):
        later = incoming * jnp.exp(tot_buf[k, 0:1, :]) + st_buf[k].astype(F32)
        incoming = jnp.where(k <= s, later, incoming)
    outside = jnp.dot(queries, incoming.astype(BF16), preferred_element_type=F32)
    g_send[...] = ((mixed + outside * reach) * modulation).astype(BF16)
    spreads = []
    for q in (2, 3, 1) if tp == 4 else range(1, tp):
        to = (t + q) % tp
        copy = remote(
            g_send.at[pl.ds(to * rows, rows)], g_buf.at[t], g_ss.at[q], g_rs.at[q], s, to
        )
        copy.start()
        spreads.append(copy)
    g_buf[t] = g_send[pl.ds(pl.multiple_of(t * rows, rows), rows), :]

    own_meta = meta_ref[...]
    onehots = []
    for k in range(n):
        first = ((s + k) % n * locals_).astype(F32)
        onehots.append(routing(own_meta, first, rows, cap, locals_).astype(BF16))
    for copy in meta_copies:
        copy.wait()
    fetches[0].wait()
    for copy in spreads:
        copy.wait()
    squares = jnp.zeros((rows, 1), F32)
    for i in range(tp):
        piece = g_buf[i].astype(F32)
        squares = squares + jnp.sum(piece * piece, axis=1, keepdims=True)
    scale = lax.rsqrt(squares / (tp * width) + EPS)
    projected = carry_ref[...].astype(F32)
    for i in range(tp):
        span = slice(i * width, (i + 1) * width)
        normed = (g_buf[i].astype(F32) * scale * gain_ref[:, span]).astype(BF16)
        projected = projected + jnp.dot(normed, blend[span, :], preferred_element_type=F32)
    middle = projected.astype(BF16)
    mid[...] = middle
    wide = middle.astype(F32)
    expert_in = (
        wide
        * lax.rsqrt(jnp.mean(wide * wide, axis=1, keepdims=True) + EPS)
        * sgain_ref[...]
    ).astype(BF16)

    order = []
    for k in range(n // 2 + 1):
        for other in (k, (n - k) % n):
            if other not in order:
                order.append(other)

    z_copies, far_copies, near_copies, p1_copies, p2_copies, ret_copies = {}, {}, {}, {}, {}, {}
    for k in order[1:] + order[:1]:
        picked = jnp.dot(onehots[k], expert_in, preferred_element_type=F32).astype(BF16)
        if k == 0:
            arr[0, t] = picked
        else:
            x_send[k] = picked
            z_copies[k] = remote(
                x_send.at[k], arr.at[k, t], z_ss.at[k], z_rs.at[k], (s + k) % n, t
            )
            z_copies[k].start()

    def pass_far(k):
        if k:
            z_copies[k].wait()
        far_copies[k] = remote(arr.at[k, t], arr.at[k, t], far_ss.at[k], far_rs.at[k], s, far)
        far_copies[k].start()
        first = remote(
            arr.at[k, t], arr.at[k, t], near_ss.at[k, 0], near_rs.at[k, 0], s, near
        )
        first.start()
        near_copies[k] = [first]

    def pass_near(k):
        far_copies[k].wait()
        second = remote(
            arr.at[k, far], arr.at[k, far], near_ss.at[k, 1], near_rs.at[k, 1], s, near
        )
        second.start()
        near_copies[k].append(second)

    weight_row0 = s * locals_

    def slot_weights(k):
        columns = [[] for _ in range(locals_)]
        for i in range(tp):
            q = (t + tp - i) % tp
            meta = metas[k, q]
            onehot = routing(meta, weight_row0.astype(F32), rows, cap, locals_)
            for l in range(locals_):
                expert = (weight_row0 + l).astype(F32)
                lift0, lift1 = jnp.exp(meta[2:3, :rows]), jnp.exp(meta[3:4, :rows])
                share = meta[4:5, :rows] / (lift0 + lift1)
                mine = share * (
                    jnp.where(meta[0:1, :rows] == expert, lift0, 0.0)
                    + jnp.where(meta[1:2, :rows] == expert, lift1, 0.0)
                )
                columns[l].append(jnp.sum(onehot * mine, axis=1, keepdims=True))
        return [jnp.concatenate(c, axis=0) for c in columns]

    def experts(k):
        shares = slot_weights(k)
        for copy in near_copies[k]:
            copy.wait()
        tokens = arr[k].reshape(tp * cap, model)
        if not loaded:
            for fetch in fetches[1:]:
                fetch.wait()
            loaded.append(True)
        total = None
        for l in range(locals_):
            gate = jnp.dot(tokens, wg[l], preferred_element_type=F32)
            up = jnp.dot(tokens, wu[l], preferred_element_type=F32)
            hidden = (silu(gate) * up * shares[l]).astype(BF16)
            term = jnp.dot(hidden, wd[l], preferred_element_type=F32)
            total = term if total is None else total + term
        part[k] = total.astype(BF16).reshape(tp, cap, model)
        pair = []
        for i, owner in ((1, near_far), (0, near)):
            copy = remote(
                part.at[k, owner], rs1.at[k, i], p1_ss.at[k, i], p1_rs.at[k, i], s, near
            )
            copy.start()
            pair.append(copy)
        p1_copies[k] = pair

    def reduce_near(k):
        for copy in p1_copies[k]:
            copy.wait()
        far_send[k] = (part[k, far].astype(F32) + rs1[k, 1].astype(F32)).astype(BF16)
        p2_copies[k] = remote(far_send.at[k], rs2.at[k], p2_ss.at[k], p2_rs.at[k], s, far)
        p2_copies[k].start()

    def reduce_far(k):
        p2_copies[k].wait()
        total = (
            part[k, t].astype(F32) + rs1[k, 0].astype(F32) + rs2[k].astype(F32)
        ).astype(BF16)
        if k == 0:
            ret[0] = total
        else:
            ret_send[k] = total
            ret_copies[k] = remote(
                ret_send.at[k], ret.at[k], ret_ss.at[k], ret_rs.at[k], (s + n - k) % n, t
            )
            ret_copies[k].start()

    loaded = []
    pass_far(order[0])
    for i in range(n + 2):
        if i + 1 < n:
            pass_far(order[i + 1])
        if i < n:
            pass_near(order[i])
            experts(order[i])
        if 0 <= i - 1 < n:
            reduce_near(order[i - 1])
        if 0 <= i - 2 < n:
            reduce_far(order[i - 2])

    result = mid[...].astype(F32)
    for k in order:
        if k:
            ret_copies[k].wait()
        result = result + first_dims(onehots[k], ret[k])
    out_ref[...] = result.astype(BF16)


def per_device(
    n,
    tp,
    carryover_vector,
    channel_source_entries,
    final_modulation_vector,
    entering_basis_matrix,
    readout_basis_matrix,
    raw_stride_amount,
    extra_log_attenuation,
    channel_fading_rate,
    channel_source_kernel,
    entering_basis_kernel,
    readout_basis_kernel,
    modulated_rescaling_vector,
    blender_final_matrix,
    specialist_rescaling_vector,
    specialist_gating_matrices,
    widening_matrices,
    contracting_matrices,
    assigned_specialist_ids,
    specialist_choice_affinity,
    cluster_chance,
):
    length, width = channel_source_entries.shape
    rows, model = carryover_vector.shape
    locals_, _, hidden = specialist_gating_matrices.shape
    experts = n * locals_
    picks = assigned_specialist_ids.shape[1]
    assert tp == 4 and picks == 2 and entering_basis_matrix.shape[1] == STATE
    per_expert = 2 * rows * picks // experts
    group_size = experts // EXPERT_GROUPS
    if group_size <= locals_:
        cap = locals_ * per_expert // picks
    else:
        cap = locals_ * per_expert
    cap = -(-min(cap, rows) // 16) * 16
    vmem = pl.BlockSpec(memory_space=pltpu.VMEM)
    hbm = pl.BlockSpec(memory_space=pl.ANY)
    dma = pltpu.SemaphoreType.DMA
    scratch = [
        pltpu.VMEM(blender_final_matrix.shape, BF16),
        pltpu.VMEM(specialist_gating_matrices.shape, BF16),
        pltpu.VMEM(widening_matrices.shape, BF16),
        pltpu.VMEM(contracting_matrices.shape, BF16),
        pltpu.VMEM((TAIL, width), BF16),
        pltpu.VMEM((TAIL, STATE), BF16),
        pltpu.VMEM((TAIL, STATE), BF16),
        pltpu.VMEM((TAIL + length, width + 2 * STATE), F32),
        pltpu.VMEM((STATE, width), BF16),
        pltpu.VMEM((8, width), F32),
        pltpu.VMEM((n, STATE, width), BF16),
        pltpu.VMEM((n, 8, width), F32),
        pltpu.VMEM((length, width), BF16),
        pltpu.VMEM((tp, rows, width), BF16),
        pltpu.VMEM((rows, model), BF16),
        pltpu.VMEM((8, 128), F32),
        pltpu.VMEM((n, tp, 8, 128), F32),
        pltpu.VMEM((n, cap, model), BF16),
        pltpu.VMEM((n, tp, cap, model), BF16),
        pltpu.VMEM((n, tp, cap, model), BF16),
        pltpu.VMEM((n, 2, cap, model), BF16),
        pltpu.VMEM((n, cap, model), BF16),
        pltpu.VMEM((n, cap, model), BF16),
        pltpu.VMEM((n, cap, model), BF16),
        pltpu.VMEM((n, cap, model), BF16),
        dma((4,)),
    ]
    for shape in ((3,), (n,), (n,), (n, tp), (tp,), (n,), (n,), (n, 2), (n, 2), (n,), (n,)):
        scratch += [dma(shape), dma(shape)]
    return pl.pallas_call(
        functools.partial(kernel, n, tp, cap),
        out_shape=jax.ShapeDtypeStruct((rows, model), BF16),
        in_specs=[vmem] * 11 + [hbm, vmem, hbm, hbm, hbm] + [vmem] * 4,
        out_specs=vmem,
        scratch_shapes=scratch,
        compiler_params=pltpu.CompilerParams(
            collective_id=0, has_side_effects=True, vmem_limit_bytes=60 * 1024 * 1024
        ),
    )(
        channel_source_entries,
        entering_basis_matrix,
        readout_basis_matrix,
        final_modulation_vector,
        raw_stride_amount.T,
        extra_log_attenuation.T,
        channel_fading_rate[:, None],
        channel_source_kernel,
        entering_basis_kernel,
        readout_basis_kernel,
        modulated_rescaling_vector[None, :],
        blender_final_matrix,
        specialist_rescaling_vector[None, :],
        specialist_gating_matrices,
        widening_matrices,
        contracting_matrices,
        assigned_specialist_ids.T,
        specialist_choice_affinity.T,
        cluster_chance[None, :],
        carryover_vector,
    )


def solution(mesh):
    return jax.shard_map(
        functools.partial(per_device, mesh.shape["sp"], mesh.shape["tp"]),
        mesh=mesh,
        in_specs=(
            P(("grp", "sp", "tp"), None),
            P(("grp", "sp"), "tp"),
            P(("grp", "sp"), "tp"),
            P(("grp", "sp"), "tp"),
            P(("grp", "sp"), "tp"),
            P(("grp", "sp"), "tp"),
            P(("grp", "sp"), "tp"),
            P("tp"),
            P(None, "tp"),
            P(None, "tp"),
            P(None, "tp"),
            P(),
            P(),
            P(),
            P("sp", None, "tp"),
            P("sp", None, "tp"),
            P("sp", "tp", None),
            P(("grp", "sp"), None),
            P(("grp", "sp", "tp"), None),
            P(("grp", "sp", "tp")),
        ),
        out_specs=P(("grp", "sp", "tp"), None),
        check_vma=False,
    )
```
